32 devices in a mesh: sp: 8 (over z, y), tp: 4 (over x, core).
Axes of the slice: x: 2, y: 2, z: 4, core: 2. Of those that a mesh axis runs over, the one named last changes fastest.
Arguments:
- hidden: bfloat16 [2048, 4096], P('sp'), as said below
- key_weight: bfloat16 [4096, 1024], P(None, 'tp'), as said below
- queries: bfloat16 [2048, 4096], P('sp', 'tp'), as said below
- values: bfloat16 [2048, 1024], P('sp', 'tp'), as said below
- map_out: bfloat16 [2048, 8192], P('sp', 'tp'), as said below
- log_sums: float32 [32, 2048], P('tp', 'sp'), as said below
- out_grad: bfloat16 [2048, 4096], P('sp', 'tp'), may hold values from -6 to 6
- mixing: float32 [16], P('tp'), may hold values from 0.3 to 0.8
- out_gain: float32 [256], replicated, may hold values from 0.1 to 1.9
Outputs:
- grad_query: bfloat16 [2048, 4096], P('sp', 'tp')
- grad_key: bfloat16 [2048, 1024], P('sp', 'tp')
- grad_value: bfloat16 [2048, 1024], P('sp', 'tp')
- grad_weight: float32 [4096, 1024], P('sp', 'tp')
The draws below stay inside these ranges and needn't reach their ends.
Inputs may be any that keep to these rules, and one draw needn't show every extreme that they name: `hidden`: inputs of order one. `key_weight`: entries of order 1 / sqrt(4096) times a constant. `queries`: entries of order one. `values`: entries of order one. `log_sums`: for head h, map m and row i: the logarithm of the sum over keys j <= i of exp(scores[h, m](i, j)), with key_rows formed as in the reference program. `map_out`: for head h and map m: the row's weights exp(scores - log_sums) over keys j <= i times the values of key head g(h), rounded to bfloat16.
All inputs are finite; a program needn't handle non-finite values.
Results may differ from the reference program's by a relative error of at most 0.02.
Values may be sent and summed in bfloat16 or wider, within the bound.
No kernel may reach another device: no remote copies, remote signals or barrier semaphores. Data moves between devices by JAX's collectives and lax.ppermute only.
A program may use at most 256 MiB of HBM per device.

```python
import math
import jax
import jax.numpy as jnp
from jax import lax

D = 4096
HEADS = 16
KV_HEADS = 4
HEAD_DIM = 128
V_DIM = 256
TOKENS = 2048


def base_arrays(key):
    key_hidden = jax.random.fold_in(key, 101)
    key_weight = jax.random.fold_in(key, 102)
    key_query = jax.random.fold_in(key, 103)
    key_value = jax.random.fold_in(key, 104)
    hidden = jax.random.normal(key_hidden, (TOKENS, D), jnp.float32)
    queries = jax.random.normal(key_query, (TOKENS, HEADS * 2 * HEAD_DIM), jnp.float32)
    weight = jax.random.normal(key_weight, (D, KV_HEADS * 2 * HEAD_DIM), jnp.float32) * (1.5 / math.sqrt(D))
    values = jax.random.normal(key_value, (TOKENS, KV_HEADS * V_DIM), jnp.float32)
    return (hidden.astype(jnp.bfloat16), weight.astype(jnp.bfloat16), queries.astype(jnp.bfloat16), values.astype(jnp.bfloat16))


def forward_arrays(key):
    hidden, weight, queries, values = base_arrays(key)
    key_rows = jnp.dot(hidden, weight, preferred_element_type=jnp.float32).astype(jnp.bfloat16).astype(jnp.float32)
    per_group = HEADS // KV_HEADS
    block_rows = 128 if TOKENS % 128 == 0 else TOKENS
    n_blocks = TOKENS // block_rows
    query_all = queries.astype(jnp.float32).reshape(n_blocks, block_rows, KV_HEADS, per_group, 2, HEAD_DIM)
    key_all = key_rows.reshape(TOKENS, KV_HEADS, 2, HEAD_DIM)
    value_all = values.astype(jnp.float32).reshape(TOKENS, KV_HEADS, V_DIM)
    positions = jnp.arange(TOKENS, dtype=jnp.int32).reshape(n_blocks, block_rows)
    key_pos = jnp.arange(TOKENS, dtype=jnp.int32)
    sums_list, outs_list = ([], [])
    for head_group in range(KV_HEADS):
        key_g = key_all[:, head_group]
        value_g = value_all[:, head_group]

        def one_block(inputs):
            query_block, query_pos = inputs
            scores = jnp.einsum('bpmd,tmd->pmbt', query_block[:, head_group], key_g) * HEAD_DIM ** (-0.5)
            visible = key_pos[None, :] <= query_pos[:, None]
            scores = jnp.where(visible, scores, -1e+30)
            row_max = jnp.max(scores, axis=-1, keepdims=True)
            log_sum = row_max + jnp.log(jnp.sum(jnp.exp(scores - row_max), axis=-1, keepdims=True))
            probs_map = jnp.exp(scores - log_sum)
            outputs = jnp.einsum('pmbt,tv->bpmv', probs_map, value_g)
            return (log_sum[..., 0], outputs)
        sums_g, outs_g = lax.map(one_block, (query_all, positions))
        sums_list.append(jnp.transpose(sums_g, (1, 2, 0, 3)).reshape(per_group * 2, TOKENS))
        outs_list.append(outs_g.reshape(TOKENS, per_group * 2 * V_DIM))
    return (jnp.concatenate(sums_list, axis=0), jnp.concatenate(outs_list, axis=1).astype(jnp.bfloat16))


def draw_hidden(key, part):
    return base_arrays(key)[0]


def draw_key_weight(key, part):
    return base_arrays(key)[1]


def draw_queries(key, part):
    return base_arrays(key)[2]


def draw_values(key, part):
    return base_arrays(key)[3]


def draw_log_sums(key, part):
    return forward_arrays(key)[0]


def draw_map_out(key, part):
    return forward_arrays(key)[1]


def spiked(entries, stream_key, source, target, blocks, factor):
    def block_of(axis_at):
        return (jnp.arange(entries.shape[axis_at]) // (entries.shape[axis_at] // blocks)).reshape((-1,) + (1,) * (entries.ndim - 1 - axis_at))

    first = jax.random.permutation(stream_key, blocks)[block_of(target)]
    second = (block_of(target) + blocks // 2) % blocks
    return jnp.where((block_of(source) == first) | (block_of(source) == second), factor * entries, entries)


def steps_of(stream_key, shape, cuts, smallest, high):
    def one(dim, blocks):
        heights = jax.random.uniform(jax.random.fold_in(jax.random.fold_in(stream_key, 6), dim), (blocks,), jnp.float32, smallest / len(cuts), high / len(cuts))
        return jnp.repeat(jnp.exp(heights), shape[dim] // blocks).reshape((-1,) + (1,) * (len(shape) - dim - 1))

    level = one(*cuts[0])
    for cut in cuts[1:]:
        level = level * one(*cut)
    return level


def bell_draw_with(own_key, extent, deviation, most, cuts, heavy, held_as=jnp.bfloat16):
    entries = deviation * jax.random.normal(own_key, extent, jnp.float32)
    if cuts:
        entries = entries * steps_of(own_key, extent, cuts, -0.22, 0.18)
    return jnp.clip(spiked(entries, jax.random.fold_in(own_key, 3), *heavy), -most, most).astype(held_as)


def setup_inputs(seed: int = 0) -> dict:
    seeds = jax.random.split(jax.random.key(seed), 10)
    hidden = draw_hidden(jax.random.fold_in(seeds[9], 71), 0)
    key_weight = draw_key_weight(jax.random.fold_in(seeds[9], 71), 0)
    queries = draw_queries(jax.random.fold_in(seeds[9], 71), 0)
    values = draw_values(jax.random.fold_in(seeds[9], 71), 0)
    map_out = draw_map_out(jax.random.fold_in(seeds[9], 71), 0)
    log_sums = draw_log_sums(jax.random.fold_in(seeds[9], 71), 0)
    out_grad = bell_draw_with(seeds[6], (TOKENS, HEADS * V_DIM), 1.0, 6.0, ((0, 8), (1, 4)), (0, 1, 8, 2.0))
    mixing = jnp.clip(0.3 + 0.5 * jax.random.uniform(seeds[7], (HEADS,), jnp.float32) ** steps_of(seeds[7], (HEADS,), ((0, 4),), -0.2, 0.2), 0.3, 0.8)
    out_gain = jnp.clip(1.0 + 0.18 * jax.random.normal(seeds[8], (V_DIM,), jnp.float32), 0.1, 1.9)
    return {"hidden": hidden, "key_weight": key_weight, "queries": queries, "values": values, "map_out": map_out, "log_sums": log_sums, "out_grad": out_grad, "mixing": mixing, "out_gain": out_gain}


OUT_SCALE = 0.8
NORM_EPS = 1e-06

def head_terms(out_grad, map_out, mixing, out_gain):
    rows_here = out_grad.shape[0]
    heads_here = mixing.shape[0]
    v_width = out_gain.shape[0]
    maps_out = map_out.astype(jnp.float32).reshape(rows_here, heads_here, 2, v_width)
    pre_norm = maps_out[:, :, 0] - mixing[None, :, None] * maps_out[:, :, 1]
    inverse = lax.rsqrt(lax.optimization_barrier(jnp.mean(pre_norm * pre_norm, axis=-1, keepdims=True)) + NORM_EPS)
    upstream = out_grad.astype(jnp.float32).reshape(rows_here, heads_here, v_width) * out_gain * OUT_SCALE
    d_out = inverse * (upstream - pre_norm * inverse * inverse * lax.optimization_barrier(jnp.mean(upstream * pre_norm, axis=-1, keepdims=True)))
    row_terms = lax.optimization_barrier(jnp.sum(d_out[:, :, None, :] * maps_out, axis=-1)).reshape(rows_here, heads_here * 2)
    return (d_out.reshape(rows_here, heads_here * v_width).astype(jnp.bfloat16), row_terms)

def round_trip(array):
    return lax.optimization_barrier(array.astype(jnp.bfloat16)).astype(jnp.float32)

def block_grads(query_blk, d_blk, log_blk, term_blk, query_pos, key_all, value_all, key_pos, mix_blk):
    scale = query_blk.shape[-1] ** (-0.5)
    log_part = jnp.transpose(log_blk, (1, 2, 3, 0))[..., None]
    term_part = jnp.transpose(term_blk, (1, 2, 3, 0))[..., None]
    scores = jnp.einsum('rgpmd,kgmd->gpmrk', query_blk, key_all) * scale
    visible = key_pos[None, :] <= query_pos[:, None]
    probs_map = jnp.exp(jnp.where(visible, scores - log_part, -1e+30))
    d_attn = jnp.einsum('rgpv,kgv->gprk', d_blk, value_all)
    mix_cols = mix_blk[:, :, None, None]
    weights_a = round_trip(probs_map[:, :, 0] - mix_cols * probs_map[:, :, 1])
    d_scores = round_trip(jnp.stack([probs_map[:, :, 0] * (d_attn - term_part[:, :, 0]), -mix_cols * probs_map[:, :, 1] * (d_attn - term_part[:, :, 1])], axis=2))
    grad_q = jnp.einsum('gpmrk,kgmd->rgpmd', d_scores, key_all) * scale
    grad_k = jnp.einsum('gpmrk,rgpmd->kgmd', d_scores, query_blk) * scale
    grad_v = jnp.einsum('gprk,rgpv->kgv', weights_a, d_blk)
    return (grad_q, grad_k, grad_v)

def reference(hidden, key_weight, queries, values, map_out, log_sums, out_grad, mixing, out_gain):
    total = queries.shape[0]
    per_group = HEADS // KV_HEADS
    key_rows = jnp.dot(hidden, key_weight, preferred_element_type=jnp.float32).astype(jnp.bfloat16)
    d_rows, row_terms = head_terms(out_grad, map_out, mixing, out_gain)
    query_all = queries.astype(jnp.float32).reshape(total, KV_HEADS, per_group, 2, HEAD_DIM)
    key_all = key_rows.astype(jnp.float32).reshape(total, KV_HEADS, 2, HEAD_DIM)
    value_all = values.astype(jnp.float32).reshape(total, KV_HEADS, V_DIM)
    d_all = d_rows.astype(jnp.float32).reshape(total, KV_HEADS, per_group, V_DIM)
    log_all = log_sums.T.reshape(total, KV_HEADS, per_group, 2)
    term_all = row_terms.reshape(total, KV_HEADS, per_group, 2)
    mix_all = mixing.reshape(KV_HEADS, per_group)
    block_rows = 256 if total % 256 == 0 else total
    n_blocks = total // block_rows
    key_pos = jnp.arange(total, dtype=jnp.int32)
    query_list, key_list, value_list = ([], [], [])
    for head_group in range(KV_HEADS):
        query_g = query_all[:, head_group:head_group + 1]
        d_g = d_all[:, head_group:head_group + 1]
        log_g = log_all[:, head_group:head_group + 1]
        term_g = term_all[:, head_group:head_group + 1]
        key_g = key_all[:, head_group:head_group + 1]
        value_g = value_all[:, head_group:head_group + 1]
        mix_g = mix_all[head_group:head_group + 1]

        def step_fn(carry, index):
            acc_key, acc_value = carry
            start = (index * block_rows).astype(jnp.int32)
            query_pos = start + jnp.arange(block_rows, dtype=jnp.int32)
            grad_q, grad_k, grad_v = block_grads(lax.dynamic_slice_in_dim(query_g, start, block_rows, 0), lax.dynamic_slice_in_dim(d_g, start, block_rows, 0), lax.dynamic_slice_in_dim(log_g, start, block_rows, 0), lax.dynamic_slice_in_dim(term_g, start, block_rows, 0), query_pos, key_g, value_g, key_pos, mix_g)
            return ((acc_key + grad_k, acc_value + grad_v), grad_q)
        init = (jnp.zeros((total, 1, 2, HEAD_DIM), jnp.float32), jnp.zeros((total, 1, V_DIM), jnp.float32))
        (acc_key, acc_value), grads_q = lax.scan(step_fn, init, jnp.arange(n_blocks, dtype=jnp.int32))
        query_list.append(grads_q.reshape(total, per_group * 2 * HEAD_DIM))
        key_list.append(acc_key.reshape(total, 2 * HEAD_DIM))
        value_list.append(acc_value.reshape(total, V_DIM))
    grad_query = jnp.concatenate(query_list, axis=1).astype(jnp.bfloat16)
    grad_key = jnp.concatenate(key_list, axis=1).astype(jnp.bfloat16)
    grad_value = jnp.concatenate(value_list, axis=1).astype(jnp.bfloat16)
    grad_weight = lax.dot_general(hidden, grad_key, (((0,), (0,)), ((), ())), preferred_element_type=jnp.float32)
    return (grad_query, grad_key, grad_value, grad_weight)
```

```python
import functools
import jax
import jax.numpy as jnp
from jax import lax
from jax.experimental import pallas as pl
from jax.experimental.pallas import tpu as pltpu
from jax.sharding import PartitionSpec as P

HEAD_DIM = 128
V_DIM = 256
OUT_SCALE = 0.8
NORM_EPS = 1e-06
F32 = jnp.float32
BF16 = jnp.bfloat16


NT = (((1,), (1,)), ((), ()))
TN = (((0,), (0,)), ((), ()))
NN = (((1,), (0,)), ((), ()))


def mm(a, b, dims):
    return lax.dot_general(a, b, dims, preferred_element_type=F32)


def head_kernel(mix_ref, grad_ref, maps_ref, gain_ref, logs_ref, d_ref, stats_ref):
    mix = mix_ref[pl.program_id(0)]
    map_a = maps_ref[:, :V_DIM].astype(F32)
    map_b = maps_ref[:, V_DIM:].astype(F32)
    pre = map_a - mix * map_b
    inv = lax.rsqrt(jnp.mean(pre * pre, axis=-1, keepdims=True) + NORM_EPS)
    up = grad_ref[...].astype(F32) * gain_ref[...] * OUT_SCALE
    d_out = inv * (up - pre * inv * inv * jnp.mean(up * pre, axis=-1, keepdims=True))
    d_ref[...] = d_out.astype(BF16)
    rows = d_out.shape[0]
    stats_ref[0, 0:2, :] = logs_ref[0]
    for at, one in ((2, map_a), (3, map_b)):
        term = jnp.sum(d_out * one, axis=-1, keepdims=True)
        stats_ref[0, at : at + 1, :] = jnp.broadcast_to(term, (rows, 128)).T[0:1, :]
    stats_ref[0, 4:8, :] = jnp.zeros((4, rows), F32)


def head_terms(out_grad, map_out, log_sums, mixing, out_gain):
    rows = out_grad.shape[0]
    heads = mixing.shape[0]
    return pl.pallas_call(
        head_kernel,
        grid=(heads,),
        in_specs=[
            pl.BlockSpec(memory_space=pltpu.SMEM),
            pl.BlockSpec((rows, V_DIM), lambda h: (0, h)),
            pl.BlockSpec((rows, 2 * V_DIM), lambda h: (0, h)),
            pl.BlockSpec((1, V_DIM), lambda h: (0, 0)),
            pl.BlockSpec((1, 2, rows), lambda h: (h, 0, 0)),
        ],
        out_specs=[
            pl.BlockSpec((rows, V_DIM), lambda h: (0, h)),
            pl.BlockSpec((1, 8, rows), lambda h: (h, 0, 0)),
        ],
        out_shape=[
            jax.ShapeDtypeStruct((rows, heads * V_DIM), BF16),
            jax.ShapeDtypeStruct((heads, 8, rows), F32),
        ],
    )(mixing, out_grad, map_out, out_gain.reshape(1, V_DIM), log_sums.reshape(heads, 2, rows))


def attend_kernel(diagonal, first, per_group, *refs):
    if first:
        (flags, mix_ref, k_ref, v_ref, q_a, d_a, s_a, q_b, d_b, s_b, gq_a, gq_b, out, acc_k, acc_v) = refs
        old = (None, None)
    else:
        (flags, mix_ref, k_ref, v_ref, q_a, d_a, s_a, q_b, d_b, s_b, old_a, old_b, gq_a, gq_b, out, acc_k, acc_v) = refs
        old = (old_a, old_b)
    head = pl.program_id(0)
    place = head % per_group
    mix = mix_ref[head]
    scale = HEAD_DIM ** (-0.5)

    @pl.when(place == 0)
    def _():
        acc_k[...] = jnp.zeros_like(acc_k)
        acc_v[...] = jnp.zeros_like(acc_v)

    def rows_of(q_ref, d_ref, s_ref, old_ref, gq_ref, masked):
        keys = k_ref[...]
        d_blk = d_ref[...]
        stats = s_ref[0]
        d_attn = mm(v_ref[...], d_blk, NT)
        weights = None
        for m in (0, 1):
            key = keys[:, m * HEAD_DIM : (m + 1) * HEAD_DIM]
            query = q_ref[:, m * HEAD_DIM : (m + 1) * HEAD_DIM]
            scores = mm(key, query, NT) * scale - stats[m : m + 1, :]
            if masked:
                at_key = lax.broadcasted_iota(jnp.int32, scores.shape, 0)
                at_row = lax.broadcasted_iota(jnp.int32, scores.shape, 1)
                scores = jnp.where(at_key <= at_row, scores, -1e30)
            probs = jnp.exp(scores)
            if m == 1:
                probs = -mix * probs
            weights = probs if m == 0 else weights + probs
            d_scores = (probs * (d_attn - stats[2 + m : 3 + m, :])).astype(BF16)
            part = mm(d_scores, key, TN)
            cols = slice(m * HEAD_DIM, (m + 1) * HEAD_DIM)
            gq_ref[:, cols] = part if old_ref is None else old_ref[:, cols] + part
            acc_k[:, cols] += mm(d_scores, query, NN)
        acc_v[...] += mm(weights.astype(BF16), d_blk, NN)

    def keep(old_ref, gq_ref):
        gq_ref[...] = jnp.zeros_like(gq_ref) if old_ref is None else old_ref[...]

    sets = ((q_a, d_a, s_a, old[0], gq_a, diagonal), (q_b, d_b, s_b, old[1], gq_b, False))
    for at, one in enumerate(sets):
        pl.when(flags[at] != 0)(functools.partial(rows_of, *one))
        pl.when(flags[at] == 0)(functools.partial(keep, one[3], one[4]))

    @pl.when(place == per_group - 1)
    def _():
        out[:, : 2 * HEAD_DIM] = (acc_k[...] * scale).astype(out.dtype)
        out[:, 2 * HEAD_DIM :] = acc_v[...].astype(out.dtype)


def attend(flags, mixing, keys, values, own, other, olds, diagonal, per_group, out_type):
    n_keys = keys.shape[0]
    rows = own[0].shape[0]
    heads = mixing.shape[0]
    groups = heads // per_group
    smem = pl.BlockSpec(memory_space=pltpu.SMEM)
    per_head = pl.BlockSpec((rows, V_DIM), lambda h: (0, h))
    stat = pl.BlockSpec((1, 8, rows), lambda h: (h, 0, 0))
    group_cols = pl.BlockSpec((n_keys, V_DIM), lambda h: (0, h // per_group))
    first = olds is None
    in_specs = [smem, smem, group_cols, group_cols] + [per_head, per_head, stat] * 2
    args = [flags, mixing, keys, values, *own, *other]
    if not first:
        in_specs += [per_head, per_head]
        args += list(olds)
    width = 2 * HEAD_DIM + V_DIM
    return pl.pallas_call(
        functools.partial(attend_kernel, diagonal, first, per_group),
        grid=(heads,),
        in_specs=in_specs,
        out_specs=[per_head, per_head, pl.BlockSpec((n_keys, width), lambda h: (0, h // per_group))],
        out_shape=[
            jax.ShapeDtypeStruct((rows, heads * V_DIM), F32),
            jax.ShapeDtypeStruct((rows, heads * V_DIM), F32),
            jax.ShapeDtypeStruct((n_keys, groups * width), out_type),
        ],
        scratch_shapes=[pltpu.VMEM((n_keys, V_DIM), F32), pltpu.VMEM((n_keys, V_DIM), F32)],
        input_output_aliases={} if first else {10: 0, 11: 1},
    )(*args)


def on_device(hidden, key_weight, queries, values, map_out, log_sums, out_grad, mixing, out_gain):
    rows = queries.shape[0]
    heads = mixing.shape[0]
    groups = values.shape[1] // V_DIM
    per_group = heads // groups
    sp_count = lax.axis_size("sp")
    tp_count = lax.axis_size("tp")
    layers = sp_count // 2
    sp_index = lax.axis_index("sp")
    tp_index = lax.axis_index("tp")
    layer = sp_index // 2
    side = sp_index % 2
    scale = HEAD_DIM ** (-0.5)

    def swap(x):
        return lax.ppermute(x, "sp", [(i, i ^ 1) for i in range(sp_count)])

    def up(x, d):
        return lax.ppermute(x, "sp", [(i, i + 2 * d) for i in range(sp_count - 2 * d)])

    def down(x, d):
        return lax.ppermute(x, "sp", [(i + 2 * d, i) for i in range(sp_count - 2 * d)])

    def turn(x, d):
        return lax.ppermute(x, "sp", [(i, (i + 2 * d) % sp_count) for i in range(sp_count)])

    def tp_swap(x, mask):
        return lax.ppermute(x, "tp", [(i, i ^ mask) for i in range(tp_count)])

    q_other = swap(queries)
    v_up = [values] + [up(values, d) for d in range(1, layers)]
    key_rows = jnp.dot(hidden, key_weight, preferred_element_type=F32).astype(BF16)
    k_up = [key_rows] + [up(key_rows, d) for d in range(1, layers)]
    d_rows, stats = head_terms(out_grad, map_out, log_sums, mixing, out_gain)
    d_other = swap(d_rows)
    s_other = swap(stats)

    share = rows // tp_count
    wide = hidden.shape[1] // layers
    pieces = []
    for d in range(layers):
        target = (layer + d) % layers
        piece = lax.dynamic_slice(hidden, (tp_index * share, target * wide), (share, wide))
        pieces.append(piece if d == 0 else turn(piece, d))
    have = jnp.stack(pieces)[:, None]
    mask = 1
    masks = []
    while mask < tp_count:
        masks.append(mask)
        mask *= 2
    for mask in masks[::-1]:
        met = tp_swap(have, mask)
        low = (tp_index & mask) == 0
        have = jnp.stack([jnp.where(low, have, met), jnp.where(low, met, have)], axis=1)
        have = have.reshape((layers, 2) + have.shape[2:])
    axes = have.ndim
    n_bits = len(masks)
    order = (0,) + tuple(range(n_bits, 0, -1)) + (axes - 3, axes - 2, axes - 1)
    column = jnp.transpose(have, order).reshape(layers * rows, wide)
    half = wide // 2
    col_own = lax.dynamic_slice_in_dim(column, side * half, half, 1)
    col_other = lax.dynamic_slice_in_dim(column, (1 - side) * half, half, 1)

    own = (queries, d_rows, stats)
    other = (q_other, d_other, s_other)
    olds = None
    arrived = []
    total = None
    for d in range(layers):
        if d == 0:
            flags = jnp.stack([jnp.int32(1), (side == 0).astype(jnp.int32)])
        else:
            here = (layer >= d).astype(jnp.int32)
            flags = jnp.stack([here, here])
        gq_own, gq_other, part = attend(
            flags, mixing, k_up[d], v_up[d], own, other, olds, d == 0, per_group, F32 if d == 0 else BF16
        )
        olds = (gq_own, gq_other)
        if d == 0:
            total = part
        else:
            arrived.append(down(part, d))
    gq_met = swap((gq_other * scale).astype(BF16))
    for part in arrived:
        total = total + part.astype(F32)
    total = total.astype(BF16).reshape(rows, groups, 2 * HEAD_DIM + V_DIM)
    grad_key = total[:, :, : 2 * HEAD_DIM].reshape(rows, groups * 2 * HEAD_DIM)
    grad_value = total[:, :, 2 * HEAD_DIM :].reshape(rows, groups * V_DIM)
    grad_query = (gq_own * scale + gq_met.astype(F32)).astype(BF16)

    keys_all = jnp.concatenate([grad_key] + [turn(grad_key, d) for d in range(1, layers)], axis=0)
    sent = swap(mm(col_other, keys_all, TN).astype(BF16))
    grad_weight = mm(col_own, keys_all, TN) + sent.astype(F32)
    return (grad_query, grad_key, grad_value, grad_weight)


def solution(mesh):
    placed = (
        P("sp", None),
        P(None, "tp"),
        P("sp", "tp"),
        P("sp", "tp"),
        P("sp", "tp"),
        P("tp", "sp"),
        P("sp", "tp"),
        P("tp"),
        P(),
    )
    return jax.shard_map(
        on_device,
        mesh=mesh,
        in_specs=placed,
        out_specs=(P("sp", "tp"), P("sp", "tp"), P("sp", "tp"), P("sp", "tp")),
        check_vma=False,
    )
```

```python
import functools
import jax
import jax.numpy as jnp
from jax import lax
from jax.experimental import pallas as pl
from jax.experimental.pallas import tpu as pltpu
from jax.sharding import PartitionSpec as P

HEAD_DIM = 128
V_DIM = 256
OUT_SCALE = 0.8
NORM_EPS = 1e-06
F32 = jnp.float32
BF16 = jnp.bfloat16


NT = (((1,), (1,)), ((), ()))
TN = (((0,), (0,)), ((), ()))
NN = (((1,), (0,)), ((), ()))


def mm(a, b, dims):
    return lax.dot_general(a, b, dims, preferred_element_type=F32)


def head_kernel(mix_ref, grad_ref, maps_ref, gain_ref, logs_ref, d_ref, stats_ref):
    mix = mix_ref[pl.program_id(0)]
    map_a = maps_ref[:, :V_DIM].astype(F32)
    map_b = maps_ref[:, V_DIM:].astype(F32)
    pre = map_a - mix * map_b
    inv = lax.rsqrt(jnp.mean(pre * pre, axis=-1, keepdims=True) + NORM_EPS)
    up = grad_ref[...].astype(F32) * gain_ref[...] * OUT_SCALE
    d_out = inv * (up - pre * inv * inv * jnp.mean(up * pre, axis=-1, keepdims=True))
    d_ref[...] = d_out.astype(BF16)
    rows = d_out.shape[0]
    for head in range(logs_ref.shape[0] // 2):

        @pl.when(pl.program_id(0) == head)
        def _(head=head):
            stats_ref[0, 0:2, :] = logs_ref[2 * head : 2 * head + 2, :]

    for at, one in ((2, map_a), (3, map_b)):
        term = jnp.sum(d_out * one, axis=-1, keepdims=True)
        stats_ref[0, at : at + 1, :] = jnp.broadcast_to(term, (rows, 128)).T[0:1, :]
    stats_ref[0, 4:8, :] = jnp.zeros((4, rows), F32)


def head_terms(out_grad, map_out, log_sums, mixing, out_gain):
    rows = out_grad.shape[0]
    heads = mixing.shape[0]
    return pl.pallas_call(
        head_kernel,
        grid=(heads,),
        in_specs=[
            pl.BlockSpec(memory_space=pltpu.SMEM),
            pl.BlockSpec((rows, V_DIM), lambda h: (0, h)),
            pl.BlockSpec((rows, 2 * V_DIM), lambda h: (0, h)),
            pl.BlockSpec((1, V_DIM), lambda h: (0, 0)),
            pl.BlockSpec((2 * heads, rows), lambda h: (0, 0)),
        ],
        out_specs=[
            pl.BlockSpec((rows, V_DIM), lambda h: (0, h)),
            pl.BlockSpec((1, 8, rows), lambda h: (h, 0, 0)),
        ],
        out_shape=[
            jax.ShapeDtypeStruct((rows, heads * V_DIM), BF16),
            jax.ShapeDtypeStruct((heads, 8, rows), F32),
        ],
    )(mixing, out_grad, map_out, out_gain.reshape(1, V_DIM), log_sums)


def attend_kernel(distance, first, per_group, *refs):
    if first:
        (at_ref, mix_ref, k_ref, v_ref, q_a, d_a, s_a, q_b, d_b, s_b, gq_a, gq_b, out_k, out_v, acc_k, acc_v) = refs
        old = (None, None)
    else:
        (at_ref, mix_ref, k_ref, v_ref, q_a, d_a, s_a, q_b, d_b, s_b, old_a, old_b, gq_a, gq_b, out_k, out_v, acc_k, acc_v) = refs
        old = (old_a, old_b)
    head = pl.program_id(0)
    place = head % per_group
    mix = mix_ref[head]
    scale = HEAD_DIM ** (-0.5)

    @pl.when(place == 0)
    def _():
        acc_k[...] = jnp.zeros_like(acc_k)
        acc_v[...] = jnp.zeros_like(acc_v)

    def rows_of(q_ref, d_ref, s_ref, old_ref, gq_ref, masked):
        keys = k_ref[...]
        d_blk = d_ref[...]
        stats = s_ref[0]
        d_attn = mm(v_ref[...], d_blk, NT)
        weights = None
        for m in (0, 1):
            key = keys[:, m * HEAD_DIM : (m + 1) * HEAD_DIM]
            query = q_ref[:, m * HEAD_DIM : (m + 1) * HEAD_DIM]
            scores = mm(key, query, NT) * scale - stats[m : m + 1, :]
            if masked:
                at_key = lax.broadcasted_iota(jnp.int32, scores.shape, 0)
                at_row = lax.broadcasted_iota(jnp.int32, scores.shape, 1)
                scores = jnp.where(at_key <= at_row, scores, -1e30)
            probs = jnp.exp(scores)
            if m == 1:
                probs = -mix * probs
            weights = probs if m == 0 else weights + probs
            d_scores = (probs * (d_attn - stats[2 + m : 3 + m, :])).astype(BF16)
            part = mm(d_scores, key, TN)
            cols = slice(m * HEAD_DIM, (m + 1) * HEAD_DIM)
            gq_ref[:, cols] = part if old_ref is None else old_ref[:, cols] + part
            acc_k[:, cols] += mm(d_scores, query, NN)
        acc_v[...] += mm(weights.astype(BF16), d_blk, NN)

    def keep(old_ref, gq_ref):
        gq_ref[...] = jnp.zeros_like(gq_ref) if old_ref is None else old_ref[...]

    index = at_ref[0]
    if distance == 0:
        sees = (index >= 0, index % 2 == 0)
    else:
        sees = (index >= 2 * distance, index >= 2 * distance)
    sets = ((q_a, d_a, s_a, old[0], gq_a, distance == 0), (q_b, d_b, s_b, old[1], gq_b, False))
    for seen, one in zip(sees, sets):
        pl.when(seen)(functools.partial(rows_of, *one))
        pl.when(jnp.logical_not(seen))(functools.partial(keep, one[3], one[4]))

    @pl.when(place == per_group - 1)
    def _():
        out_k[...] = (acc_k[...] * scale).astype(out_k.dtype)
        out_v[...] = acc_v[...].astype(out_v.dtype)


def attend(place, mixing, kv, own, other, olds, distance, per_group, out_type):
    n_keys = kv.shape[0]
    rows = own[0].shape[0]
    heads = mixing.shape[0]
    groups = heads // per_group
    smem = pl.BlockSpec(memory_space=pltpu.SMEM)
    per_head = pl.BlockSpec((rows, V_DIM), lambda h: (0, h))
    stat = pl.BlockSpec((1, 8, rows), lambda h: (h, 0, 0))
    group_cols = pl.BlockSpec((n_keys, V_DIM), lambda h: (0, h // per_group))
    first = olds is None
    value_cols = pl.BlockSpec((n_keys, V_DIM), lambda h: (0, groups + h // per_group))
    in_specs = [smem, smem, group_cols, value_cols] + [per_head, per_head, stat] * 2
    args = [place, mixing, kv, kv, *own, *other]
    if not first:
        in_specs += [per_head, per_head]
        args += list(olds)
    return pl.pallas_call(
        functools.partial(attend_kernel, distance, first, per_group),
        grid=(heads,),
        in_specs=in_specs,
        out_specs=[per_head, per_head, group_cols, group_cols],
        out_shape=[
            jax.ShapeDtypeStruct((rows, heads * V_DIM), F32),
            jax.ShapeDtypeStruct((rows, heads * V_DIM), F32),
            jax.ShapeDtypeStruct((n_keys, groups * V_DIM), out_type),
            jax.ShapeDtypeStruct((n_keys, groups * V_DIM), out_type),
        ],
        scratch_shapes=[pltpu.VMEM((n_keys, V_DIM), F32), pltpu.VMEM((n_keys, V_DIM), F32)],
        input_output_aliases={} if first else {10: 0, 11: 1},
    )(*args)


def on_device(hidden, key_weight, queries, values, map_out, log_sums, out_grad, mixing, out_gain):
    rows = queries.shape[0]
    heads = mixing.shape[0]
    groups = values.shape[1] // V_DIM
    per_group = heads // groups
    sp_count = lax.axis_size("sp")
    tp_count = lax.axis_size("tp")
    layers = sp_count // 2
    sp_index = lax.axis_index("sp")
    tp_index = lax.axis_index("tp")
    layer = sp_index // 2
    side = sp_index % 2
    scale = HEAD_DIM ** (-0.5)

    def swap(x):
        return lax.ppermute(x, "sp", [(i, i ^ 1) for i in range(sp_count)])

    def up(x, d):
        return lax.ppermute(x, "sp", [(i, i + 2 * d) for i in range(sp_count - 2 * d)])

    def down(x, d):
        return lax.ppermute(x, "sp", [(i + 2 * d, i) for i in range(sp_count - 2 * d)])

    def turn(x, d):
        return lax.ppermute(x, "sp", [(i, (i + 2 * d) % sp_count) for i in range(sp_count)])

    def tp_swap(x, mask):
        return lax.ppermute(x, "tp", [(i, i ^ mask) for i in range(tp_count)])

    q_other = swap(queries)
    d_rows, stats = head_terms(out_grad, map_out, log_sums, mixing, out_gain)
    d_other = swap(d_rows)
    s_other = swap(stats)
    key_rows = jnp.dot(hidden, key_weight, preferred_element_type=F32).astype(BF16)
    kv_here = jnp.concatenate([key_rows, values], axis=1)
    kv_up = [kv_here]
    for d in range(1, layers):
        kv_up.append(up(kv_here, d))
    hidden = lax.optimization_barrier((hidden, key_rows, d_rows))[0]

    share = rows // tp_count
    wide = hidden.shape[1] // layers
    pieces = []
    for d in range(layers):
        target = (layer + d) % layers
        piece = lax.dynamic_slice(hidden, (tp_index * share, target * wide), (share, wide))
        pieces.append(piece if d == 0 else turn(piece, d))
    have = jnp.stack(pieces)[:, None]
    mask = 1
    masks = []
    while mask < tp_count:
        masks.append(mask)
        mask *= 2
    for mask in masks[::-1]:
        met = tp_swap(have, mask)
        low = (tp_index & mask) == 0
        have = jnp.stack([jnp.where(low, have, met), jnp.where(low, met, have)], axis=1)
        have = have.reshape((layers, 2) + have.shape[2:])
    axes = have.ndim
    n_bits = len(masks)
    order = (0,) + tuple(range(n_bits, 0, -1)) + (axes - 3, axes - 2, axes - 1)
    column = jnp.transpose(have, order).reshape(layers * rows, wide)
    half = wide // 2
    col_own = lax.dynamic_slice_in_dim(column, side * half, half, 1)
    col_other = lax.dynamic_slice_in_dim(column, (1 - side) * half, half, 1)

    own = (queries, d_rows, stats)
    other = (q_other, d_other, s_other)
    place = sp_index.astype(jnp.int32).reshape(1)
    olds = None
    met_k, met_v = ([], [])
    for d in range(layers):
        gq_own, gq_other, part_k, part_v = attend(
            place, mixing, kv_up[d], own, other, olds, d, per_group, F32 if d == 0 else BF16
        )
        olds = (gq_own, gq_other)
        if d == 0:
            sum_k, sum_v = (part_k, part_v)
        else:
            met_k.append(down(part_k, d))
            met_v.append(down(part_v, d))
    gq_met = swap((gq_other * scale).astype(BF16))
    for part in met_k:
        sum_k = sum_k + part.astype(F32)
    grad_key = sum_k.astype(BF16)
    pieces = [grad_key]
    for d in range(1, layers):
        pieces.append(turn(grad_key, d))
    keys_all = jnp.concatenate(pieces, axis=0)
    sent = swap(mm(col_other, keys_all, TN).astype(BF16))
    grad_weight = mm(col_own, keys_all, TN) + sent.astype(F32)
    for part in met_v:
        sum_v = sum_v + part.astype(F32)
    grad_value = sum_v.astype(BF16)
    grad_query = (gq_own * scale + gq_met.astype(F32)).astype(BF16)
    return (grad_query, grad_key, grad_value, grad_weight)


def solution(mesh):
    placed = (
        P("sp", None),
        P(None, "tp"),
        P("sp", "tp"),
        P("sp", "tp"),
        P("sp", "tp"),
        P("tp", "sp"),
        P("sp", "tp"),
        P("tp"),
        P(),
    )
    return jax.shard_map(
        on_device,
        mesh=mesh,
        in_specs=placed,
        out_specs=(P("sp", "tp"), P("sp", "tp"), P("sp", "tp"), P("sp", "tp")),
        check_vma=False,
    )
```
